32 devices in a mesh: sp: 16 (over z, y, x), tp: 2 (over core).
Axes of the slice: x: 2, y: 2, z: 4, core: 2. Of those that a mesh axis runs over, the one named last changes fastest.
Arguments:
- stream: bfloat16 [4096, 2048], P(('sp', 'tp')), may hold values from -6 to 6
- outer_gate: bfloat16 [4096, 1024], P('sp', 'tp'), may hold values from -6 to 6
- inner_gate: bfloat16 [4096, 1024], P('sp', 'tp'), may hold values from -6 to 6
- conv_values: bfloat16 [4096, 1024], P('sp', 'tp'), may hold values from -6 to 6
- doc_ids: int32 [4096], P('sp'), may hold values from 0 to 7, never falling along the last dimension, each value on 1 to 1024 neighbouring positions
- conv_taps: float32 [3, 1024], P(None, 'tp'), may hold values from -3.5 to 3.5
- out_weight: bfloat16 [1024, 2048], replicated, may hold values from -0.1875 to 0.1875
- norm_gain: float32 [2048], replicated, may hold values from 0.1 to 1.9
- route_ids: int32 [4096, 2], P(('sp', 'tp')), may hold values from 0 to 31, all different within a row; in each aligned block of 128 rows (0 to 127, 128 to 255, ...) at most 16 rows name the same one
- route_logits: float32 [4096, 2], P(('sp', 'tp')), may hold values from -4 to 4
- group_weight: float32 [4096], P(('sp', 'tp')), may hold values from 0.25 to 1
- w_gate: bfloat16 [32, 2048, 1024], P(('sp', 'tp')), may hold values from -0.125 to 0.125
- w_up: bfloat16 [32, 2048, 1024], P(('sp', 'tp')), may hold values from -0.125 to 0.125
- w_down: bfloat16 [32, 1024, 2048], P(('sp', 'tp')), may hold values from -0.1875 to 0.1875
Outputs:
- result: bfloat16 [4096, 2048], P(('sp', 'tp'))
The draws below stay inside these ranges and needn't reach their ends.
Inputs may be any that keep to these rules, and one draw needn't show every extreme that they name: `route_ids`: the two experts of a token differ. In the rows of one device (aligned blocks of 128 rows) no expert is named more than 16 times, a bound that some block reaches. `doc_ids`: document numbers never fall along the sequence; a document has 1 to 1024 positions and one has exactly 1024.
All inputs are finite; a program needn't handle non-finite values.
Results may differ from the reference program's by a relative error of at most 0.0052.
Values may be sent and summed in bfloat16 or wider, within the bound.
A program may use at most 64 MiB of HBM per device.

```python
import math
import jax
import jax.numpy as jnp
import numpy as np
from jax import lax

D = 2048
CW = 1024
FF = 1024
TOPK = 2
ROWS = 128
TOKENS = 4096
EXPERTS = 32
CAP = 16
DOCS = 8
MOST_DOC = 1024


def levels(key, shape, cuts, least, high):
    def one(axis_at, shards_of):
        steps = jax.random.uniform(jax.random.fold_in(jax.random.fold_in(key, 6), axis_at), (shards_of,), jnp.float32, least / len(cuts), high / len(cuts))
        return jnp.repeat(jnp.exp(steps), shape[axis_at] // shards_of).reshape((-1,) + (1,) * (len(shape) - axis_at - 1))

    level = one(*cuts[0])
    for cut in cuts[1:]:
        level = level * one(*cut)
    return level


def length_profile(number_of, total, limit, lean):
    portions = [(1 << 20) // math.isqrt(grade ** lean) + 1 for grade in range(2, number_of + 1)]
    surplus, given = total - limit - (number_of - 1), [1] * (number_of - 1)
    while surplus > 0:
        movable = [i for i in range(number_of - 1) if given[i] < limit]
        mass, budget = sum([portions[i] for i in movable]), surplus
        for i in movable:
            extra = min(limit - given[i], max(1, budget * portions[i] // mass), surplus)
            given[i] = given[i] + extra
            surplus = surplus - extra
    return np.array([limit] + given)


def ragged(stream_key, count, total, bound, lean):
    if count == 2:
        one = jax.random.randint(stream_key, (), max(1, total - bound), min(bound, total - 1) + 1)
        return jnp.stack([one, total - one])
    tallies = jnp.asarray(length_profile(count, total, bound, lean), jnp.int32)
    twos = (count - 1) // 2
    giver, taker = tallies[1:1 + 2 * twos:2], tallies[2:2 + 2 * twos:2]
    margin = jnp.minimum(giver - 1, bound - taker)
    passed = jax.random.randint(jax.random.fold_in(stream_key, 1), (twos,), 0, 1 << 20) % (margin + 1)
    tallies = tallies.at[1:1 + 2 * twos:2].set(giver - passed).at[2:2 + 2 * twos:2].set(taker + passed)
    return tallies[jax.random.permutation(jax.random.fold_in(stream_key, 2), count)]


def routed_block(rng, own, number, rows, amount, top, bound, slope):
    sequence = jax.random.permutation(rng, amount)
    packed, ordinary = portions_of(amount, rows * top, bound, slope, True), portions_of(amount, rows * top, bound, slope, False)
    places = jnp.arange(amount)

    def named(sizes, turn):
        used = int((sizes > 0).sum())
        fixed = max(1, used // 4)
        passed = fixed + (places - fixed + turn * (used - fixed)) % max(1, amount - fixed)
        return jnp.zeros((amount,), jnp.int32).at[sequence[jnp.where(places < fixed, places, passed)]].set(jnp.asarray(sizes, jnp.int32))

    sizes = jnp.where(number % 4 == 0, named(packed, number // 4), named(ordinary, number - number // 4 - 1))
    mixed = jax.random.permutation(jax.random.fold_in(own, 3), amount)
    donor, taker = mixed[0:amount // 2 * 2:2], mixed[1:amount // 2 * 2:2]
    slack = jnp.minimum(sizes[donor] - 1, bound - sizes[taker]) // 2
    slack = jnp.where((donor == sequence[0]) | (taker == sequence[0]) | (sizes[taker] == 0), 0, jnp.maximum(slack, 0))
    passed = jax.random.randint(jax.random.fold_in(own, 4), (amount // 2,), 0, 1 << 20) % (slack + 1)
    sizes = sizes.at[donor].add(-passed).at[taker].add(passed)
    members = jnp.searchsorted(jnp.cumsum(sizes), jnp.arange(rows * top), side="right").astype(jnp.int32)
    grid = members.reshape(top, rows).T
    grid = grid[jax.random.permutation(jax.random.fold_in(own, 1), rows)]
    turn = jax.random.randint(jax.random.fold_in(own, 2), (rows, 1), 0, top)
    return jnp.take_along_axis(grid, (jnp.arange(top)[None, :] + turn) % top, axis=1)


def portions_of(count, total, bound, lean, full):
    loads = [(1 << 20) // math.isqrt(rank ** lean) + 1 for rank in range(1, count + 1)]
    largest = bound if full else min(bound, max(-(-total // count), total * loads[0] // sum(loads)))
    least = 1 if total - largest >= count - 1 else 0
    counts, surplus = [largest] + [least] * (count - 1), total - largest - least * (count - 1)
    while surplus > 0:
        candidates = [i for i in range(1, count) if counts[i] < largest] or [i for i in range(1, count) if counts[i] < bound]
        mass, remaining = sum([loads[i] for i in candidates]), surplus
        for i in candidates:
            extra = min(bound - counts[i], max(1, remaining * loads[i] // mass), surplus)
            counts[i] = counts[i] + extra
            surplus = surplus - extra
    return np.array(counts)


def noise(stream_key, dims, deviation, bound, pieces=(), held_as=jnp.bfloat16):
    result = jax.random.normal(stream_key, dims, jnp.float32) * deviation
    if len(pieces) > 0:
        result = levels(stream_key, dims, pieces, -0.22, 0.18) * result
    return jnp.clip(result, min=-bound, max=bound).astype(held_as)


def setup_inputs(seed: int = 0) -> dict:
    arg_keys = jax.random.split(jax.random.key(seed), 15)
    stream = noise(arg_keys[0], (TOKENS, D), 1.0, 6.0, ((0, 32),))
    outer_gate = noise(arg_keys[1], (TOKENS, CW), 1.0, 6.0, ((0, 16), (1, 2)))
    inner_gate = noise(arg_keys[2], (TOKENS, CW), 1.0, 6.0, ((0, 16), (1, 2)))
    conv_values = noise(arg_keys[3], (TOKENS, CW), 1.0, 6.0, ((0, 16), (1, 2)))
    doc_ids = jnp.searchsorted(jnp.cumsum(ragged(arg_keys[4], DOCS, TOKENS, MOST_DOC, 1)), jnp.arange(TOKENS), side="right").astype(jnp.int32)
    conv_taps = noise(arg_keys[5], (3, CW), 3 ** -0.5, 3.5, ((1, 2),), jnp.float32)
    out_weight = noise(arg_keys[6], (CW, D), CW ** -0.5, 0.1875)
    norm_gain = jnp.clip(1.0 + 0.18 * jax.random.normal(arg_keys[7], (D,), jnp.float32), 0.1, 1.9)
    route_ids_keys = jax.random.split(jax.random.fold_in(arg_keys[8], 1), TOKENS // ROWS)
    route_ids_turns = jax.random.permutation(jax.random.fold_in(arg_keys[8], 3), TOKENS // ROWS)
    route_ids = jax.vmap(lambda own, number: routed_block(jax.random.fold_in(arg_keys[8], 2), own, number, ROWS, EXPERTS, TOPK, CAP, 2))(route_ids_keys, route_ids_turns).reshape((TOKENS, TOPK))
    route_logits = noise(arg_keys[9], (TOKENS, TOPK), 1.5, 4.0, ((0, 32),), jnp.float32)
    group_weight = jnp.clip(jnp.exp(math.log(1.0) - 1.3862944 * jax.random.uniform(arg_keys[10], (TOKENS,), jnp.float32) ** levels(arg_keys[10], (TOKENS,), ((0, 32),), -0.2, 0.2)), 0.25, 1.0)
    w_gate = noise(arg_keys[11], (EXPERTS, D, FF), D ** -0.5, 0.125, ((0, 32),))
    w_up = noise(arg_keys[12], (EXPERTS, D, FF), D ** -0.5, 0.125, ((0, 32),))
    w_down = noise(arg_keys[13], (EXPERTS, FF, D), FF ** -0.5, 0.1875, ((0, 32),))
    return {"stream": stream, "outer_gate": outer_gate, "inner_gate": inner_gate, "conv_values": conv_values, "doc_ids": doc_ids, "conv_taps": conv_taps, "out_weight": out_weight, "norm_gain": norm_gain, "route_ids": route_ids, "route_logits": route_logits, "group_weight": group_weight, "w_gate": w_gate, "w_up": w_up, "w_down": w_down}


def reference(stream, outer_gate, inner_gate, conv_values, doc_ids, conv_taps, out_weight, norm_gain, route_ids, route_logits, group_weight, w_gate, w_up, w_down):
    product = (inner_gate.astype(jnp.float32) * conv_values.astype(jnp.float32)).astype(jnp.bfloat16)
    prod_f = product.astype(jnp.float32)
    padded = jnp.pad(prod_f, ((1, 1), (0, 0)))
    padded_docs = jnp.pad(doc_ids, (1, 1), constant_values=-1)
    same_prev = (padded_docs[:-2] == doc_ids).astype(jnp.float32)[:, None]
    same_next = (padded_docs[2:] == doc_ids).astype(jnp.float32)[:, None]
    conv = conv_taps[0] * padded[:-2] * same_prev + conv_taps[1] * prod_f + conv_taps[2] * padded[2:] * same_next
    mixed = (outer_gate.astype(jnp.float32) * conv).astype(jnp.bfloat16)
    resid = stream.astype(jnp.float32) + jnp.dot(mixed, out_weight, preferred_element_type=jnp.float32)
    scale = lax.rsqrt(lax.optimization_barrier(jnp.mean(resid * resid, axis=-1, keepdims=True)) + 1e-06)
    normed = (resid * scale * norm_gain).astype(jnp.bfloat16)
    expo = jnp.exp(route_logits)
    gate = group_weight[:, None] * expo / lax.optimization_barrier(jnp.sum(expo, axis=1, keepdims=True))
    flat_ids = route_ids.reshape(-1)
    gate_flat = gate.reshape(-1)
    load = EXPERTS * CAP
    count_all = flat_ids.shape[0]

    def step(total, expert):
        is_hit = flat_ids == expert
        rank = jnp.cumsum(is_hit.astype(jnp.int32)) - 1
        where_to = jnp.where(is_hit, rank, load).astype(jnp.int32)
        pick = jnp.zeros((load,), jnp.int32).at[where_to].set(jnp.arange(count_all, dtype=jnp.int32), mode='drop')
        is_live = jnp.zeros((load,), gate_flat.dtype).at[where_to].set(1.0, mode='drop')
        token_of = pick // TOPK
        rows_in = normed[token_of]
        hidden = (jax.nn.silu(jnp.dot(rows_in, w_gate[expert], preferred_element_type=jnp.float32)) * jnp.dot(rows_in, w_up[expert], preferred_element_type=jnp.float32)).astype(jnp.bfloat16)
        expert_out = jnp.dot(hidden, w_down[expert], preferred_element_type=jnp.float32).astype(jnp.bfloat16)
        weights = gate_flat[pick] * is_live
        total = total.at[token_of].add(expert_out.astype(jnp.float32) * weights[:, None])
        return (total, None)
    total, unused = lax.scan(step, resid, jnp.arange(EXPERTS, dtype=jnp.int32))
    return total.astype(jnp.bfloat16)
```

```python
import functools

import jax
import jax.numpy as jnp
from jax import lax
from jax.experimental import pallas as pl
from jax.experimental.pallas import tpu as pltpu
from jax.sharding import PartitionSpec as P


def padded_2(shard, sides, width):
    for axis, dim in sides:
        size, length = (lax.axis_size(axis), shard.shape[dim])
        up = [(i, (i + 1) % size) for i in range(size - 1)]
        down = [(j, i) for i, j in up]
        last = lax.slice_in_dim(shard, length - width, length, axis=dim)
        leading = lax.slice_in_dim(shard, 0, width, axis=dim)
        before = lax.ppermute(last, axis, up)
        after = lax.ppermute(leading, axis, down)
        shard = jnp.concatenate([before, shard, after], axis=dim)
    return shard


def on_device(
    stream,
    outer_gate,
    inner_gate,
    conv_values,
    doc_ids,
    conv_taps,
    out_weight,
    norm_gain,
    route_ids,
    route_logits,
    group_weight,
    w_gate,
    w_up,
    w_down,
):
    tok_rows = stream.shape[0]
    width = stream.shape[1]
    product = (inner_gate.astype(jnp.float32) * conv_values.astype(jnp.float32)).astype(
        jnp.bfloat16
    )
    doc_float = doc_ids.astype(jnp.bfloat16)
    padded, padded_docs = (padded_2(product, (("sp", 0),), 1), padded_2(doc_float, (("sp", 0),), 1))
    same_prev = (padded_docs[:-2] == doc_float).astype(jnp.float32)[:, None]
    same_next = (padded_docs[2:] == doc_float).astype(jnp.float32)[:, None]
    conv = (
        conv_taps[0] * padded[:-2].astype(jnp.float32) * same_prev
        + conv_taps[1] * product.astype(jnp.float32)
        + conv_taps[2] * padded[2:].astype(jnp.float32) * same_next
    )
    mixed = (outer_gate.astype(jnp.float32) * conv).astype(jnp.bfloat16)
    channels = lax.all_to_all(mixed, "tp", split_axis=0, concat_axis=1, tiled=True)
    projected = jnp.dot(channels, out_weight, preferred_element_type=jnp.float32)
    resid = stream.astype(jnp.float32) + projected
    scale = lax.rsqrt(jnp.mean(resid * resid, axis=-1, keepdims=True) + 1e-06)
    normed = (resid * scale * norm_gain).astype(jnp.bfloat16)
    expert_total = lax.axis_size("sp") * lax.axis_size("tp")
    top_count = route_ids.shape[1]
    capacity = 2 * tok_rows * top_count // expert_total
    flat_ids = route_ids.reshape(-1)
    one_hot = (flat_ids[:, None] == jnp.arange(expert_total, dtype=jnp.int32)[None, :]).astype(
        jnp.int32
    )
    rank = jnp.sum((jnp.cumsum(one_hot, axis=0) - 1) * one_hot, axis=1)
    slot = flat_ids * capacity + rank
    slot_count = expert_total * capacity
    source_row = (
        jnp.zeros((slot_count,), jnp.int32)
        .at[slot]
        .set(jnp.arange(flat_ids.shape[0], dtype=jnp.int32) // top_count)
    )
    filled = jnp.zeros((slot_count,), jnp.bool_).at[slot].set(True)
    outgoing = jnp.where(filled[:, None], normed[source_row], jnp.zeros((), jnp.bfloat16)).reshape(
        expert_total, capacity, width
    )
    arrived = lax.all_to_all(outgoing, ("sp", "tp"), split_axis=0, concat_axis=0, tiled=True)
    sources, items, features = arrived.shape
    rows_in = arrived.reshape(sources * items, features)
    hidden = (
        jax.nn.silu(jnp.dot(rows_in, w_gate[0], preferred_element_type=jnp.float32))
        * jnp.dot(rows_in, w_up[0], preferred_element_type=jnp.float32)
    ).astype(jnp.bfloat16)
    outputs = jnp.dot(hidden, w_down[0], preferred_element_type=jnp.float32).astype(jnp.bfloat16)
    returned = lax.all_to_all(
        outputs.reshape(sources, items, features),
        ("sp", "tp"),
        split_axis=0,
        concat_axis=0,
        tiled=True,
    )
    picked = (
        returned.reshape(slot_count, width)[slot]
        .astype(jnp.float32)
        .reshape(tok_rows, top_count, width)
    )
    expo = jnp.exp(route_logits)
    gate = group_weight[:, None] * expo / jnp.sum(expo, axis=1, keepdims=True)
    result = resid + jnp.sum(gate[:, :, None] * picked, axis=1)
    return result.astype(jnp.bfloat16)


MESH = pl.DeviceIdType.MESH
F32, BF16 = jnp.float32, jnp.bfloat16


def dot(a, b):
    return jnp.dot(a, b, preferred_element_type=F32)


def flip(z, g):
    return 2 * ((z // 2 + g // 2) % 2) + (z % 2 + g % 2) % 2


def fused_kernel(
    tp_size, planes, per_plane, cap,
    stream, outer, inner, values, docs, taps, gain, ids, logits, weight,
    ow_hbm, wg_hbm, wu_hbm, wd_hbm,
    out,
    ow, wg, wu, wd, edge_out, edge_in, doc_in, mix, mix_in, resid, normed, hidden,
    send, recv, outb, ret,
    load_sem, edge_send, edge_recv, mix_send, mix_recv, self_sem,
    out_sem, in_sem, back_sem, home_sem,
):
    sp, tp = lax.axis_index("sp"), lax.axis_index("tp")
    sp_size = planes * per_plane // tp_size
    total = planes * per_plane
    me = sp * tp_size + tp
    z, p = me // per_plane, me % per_plane
    rows, width = stream.shape
    chan = inner.shape[1]
    length = inner.shape[0]

    def place(index):
        return (index // tp_size, index % tp_size)

    loads = [
        pltpu.make_async_copy(src, dst, load_sem.at[i])
        for i, (src, dst) in enumerate(
            ((ow_hbm, ow), (wg_hbm.at[0], wg), (wu_hbm.at[0], wu), (wd_hbm.at[0], wd))
        )
    ]
    for load in loads:
        load.start()

    barrier = pltpu.get_barrier_semaphore()

    def greet(i, carry):
        pl.semaphore_signal(
            barrier, inc=1, device_id=place((me + i) % total), device_id_type=MESH
        )
        return carry

    lax.fori_loop(1, total, greet, 0)
    product = (inner[...].astype(F32) * values[...].astype(F32)).astype(BF16)
    edge_out[0] = product[:16]
    edge_out[1] = product[length - 16 :]
    pl.semaphore_wait(barrier, total - 1)

    left, right = ((sp + sp_size - 1) % sp_size, tp), ((sp + 1) % sp_size, tp)
    edges = []
    for side, (dest, src) in enumerate(((right, edge_out.at[1]), (left, edge_out.at[0]))):
        for kind, (source, target) in enumerate(
            ((src, edge_in.at[side]), (docs, doc_in.at[side]))
        ):
            edges.append(
                pltpu.make_async_remote_copy(
                    src_ref=source,
                    dst_ref=target,
                    send_sem=edge_send.at[2 * side + kind],
                    recv_sem=edge_recv.at[2 * side + kind],
                    device_id=dest,
                    device_id_type=MESH,
                )
            )
    for edge in edges:
        edge.start()

    logit = logits[...]
    top = logit.shape[0]
    expo = jnp.exp(logit)
    gates = weight[...] * expo / jnp.sum(expo, axis=0, keepdims=True)
    gate_cols = [
        jnp.transpose(jnp.broadcast_to(gates[k : k + 1], (rows, rows)))[:, :1]
        for k in range(top)
    ]
    before = (
        lax.broadcasted_iota(jnp.int32, (rows, rows), 0)
        < lax.broadcasted_iota(jnp.int32, (rows, rows), 1)
    ).astype(F32).astype(BF16)
    id_rows = [ids[k : k + 1, :] for k in range(top)]
    rank_of = lax.broadcasted_iota(jnp.int32, (per_plane, cap, rows), 1).astype(F32)

    def slots(plane):
        expert = lax.broadcasted_iota(jnp.int32, (per_plane, rows), 0) + plane * per_plane
        hits = [(row == expert).astype(F32) for row in id_rows]
        named = sum(hits)
        ahead = dot(named.astype(BF16), before)

        def spread(hit):
            at = jnp.where(hit > 0, ahead, -1.0)
            grid = jnp.broadcast_to(at[:, None, :], (per_plane, cap, rows))
            return jnp.where(grid == rank_of, 1.0, 0.0).reshape(per_plane * cap, rows)

        return named, hits, spread

    for edge in edges:
        edge.wait()

    doc = jnp.broadcast_to(docs[...], (8, length))
    lane = lax.broadcasted_iota(jnp.int32, (8, length), 1)
    prior = jnp.where(
        lane == 0,
        pltpu.roll(jnp.broadcast_to(doc_in[0], (8, length)), 1, axis=1),
        pltpu.roll(doc, 1, axis=1),
    )
    later = jnp.where(
        lane == length - 1,
        pltpu.roll(jnp.broadcast_to(doc_in[1], (8, length)), length - 1, axis=1),
        pltpu.roll(doc, length - 1, axis=1),
    )
    spot = lane + sp * length
    same_prev = jnp.where((prior == doc) & (spot > 0), 1.0, 0.0)
    same_next = jnp.where((later == doc) & (spot < sp_size * length - 1), 1.0, 0.0)

    def column(row):
        return jnp.transpose(jnp.broadcast_to(row[:1], (128, length)))[:, :1]

    prod = product.astype(F32)
    row_at = lax.broadcasted_iota(jnp.int32, (length, chan), 0)
    prev = jnp.where(row_at == 0, edge_in[0].astype(F32)[15:16], pltpu.roll(prod, 1, axis=0))
    nxt = jnp.where(
        row_at == length - 1,
        edge_in[1].astype(F32)[:1],
        pltpu.roll(prod, length - 1, axis=0),
    )
    conv = (
        taps[0:1] * prev * column(same_prev)
        + taps[1:2] * prod
        + taps[2:3] * nxt * column(same_next)
    )
    mixed = (outer[...].astype(F32) * conv).astype(BF16)
    mix[...] = mixed.reshape(tp_size, rows, chan)
    other = 1 - tp
    swap = pltpu.make_async_remote_copy(
        src_ref=mix.at[other],
        dst_ref=mix_in,
        send_sem=mix_send,
        recv_sem=mix_recv,
        device_id=(sp, other),
        device_id_type=MESH,
    )
    swap.start()
    loads[0].wait()
    tile = 512
    own = mix[tp]
    for c in range(0, width, tile):
        resid[:, c : c + tile] = stream[:, c : c + tile].astype(F32) + dot(
            own, ow[pl.ds(pl.multiple_of(tp * chan, chan), chan), c : c + tile]
        )
    swap.wait()
    theirs = mix_in[...]
    squares = jnp.zeros((rows, 1), F32)
    for c in range(0, width, tile):
        part = resid[:, c : c + tile] + dot(
            theirs, ow[pl.ds(pl.multiple_of(other * chan, chan), chan), c : c + tile]
        )
        resid[:, c : c + tile] = part
        squares = squares + jnp.sum(part * part, axis=1, keepdims=True)
    scale = lax.rsqrt(squares / width + 1e-06)
    for c in range(0, width, tile):
        normed[:, c : c + tile] = (
            resid[:, c : c + tile] * scale * gain[:, c : c + tile]
        ).astype(BF16)

    def group_copy(src, dst, g, i, source_sem, target_sem):
        peer = (p + i) % per_plane
        return pltpu.make_async_remote_copy(
            src_ref=src.at[g, peer],
            dst_ref=dst.at[g, p],
            send_sem=source_sem.at[g],
            recv_sem=target_sem.at[g],
            device_id=place(flip(z, g) * per_plane + peer),
            device_id_type=MESH,
        )

    def start_group(src, dst, g, source_sem, target_sem):
        def one(i, carry):
            @pl.when(g * per_plane + i > 0)
            def _():
                group_copy(src, dst, g, i, source_sem, target_sem).start()

            return carry

        lax.fori_loop(0, per_plane, one, 0)

    def wait_group(buf, g, sem):
        @pl.when(g == 0)
        def _():
            part = buf.at[0, pl.ds(0, per_plane - 1)]
            pltpu.make_async_copy(part, part, sem.at[0]).wait()

        @pl.when(g > 0)
        def _():
            pltpu.make_async_copy(buf.at[g], buf.at[g], sem.at[g]).wait()

    def dispatch(n, carry):
        g = planes - 1 - n
        named, hits, spread = slots(flip(z, g))
        pick = spread(named).astype(BF16)
        for c in range(0, width, tile):
            send[g, :, :, c : c + tile] = (
                dot(pick, normed[:, c : c + tile])
                .astype(BF16)
                .reshape(per_plane, cap, tile)
            )
        start_group(send, recv, g, out_sem, in_sem)
        return carry

    lax.fori_loop(0, planes, dispatch, 0)
    keep = pltpu.make_async_copy(send.at[0, p], recv.at[0, p], self_sem)
    keep.start()
    keep.wait()
    for load in loads[1:]:
        load.wait()

    def experts(g, carry):
        wait_group(recv, g, in_sem)
        x = recv[g].reshape(per_plane * cap, width)
        ff = hidden.shape[1]
        for f in range(0, ff, 256):
            a = dot(x, wg[:, f : f + 256])
            b = dot(x, wu[:, f : f + 256])
            hidden[:, f : f + 256] = (a / (1.0 + jnp.exp(-a)) * b).astype(BF16)
        h = hidden[...]
        for c in range(0, width, tile):
            outb[g, :, :, c : c + tile] = (
                dot(h, wd[:, c : c + tile]).astype(BF16).reshape(per_plane, cap, tile)
            )
        start_group(outb, ret, g, back_sem, home_sem)
        return carry

    lax.fori_loop(0, planes, experts, 0)
    keep_back = pltpu.make_async_copy(outb.at[0, p], ret.at[0, p], self_sem)
    keep_back.start()
    keep_back.wait()

    def combine(g, carry):
        wait_group(ret, g, home_sem)
        named, hits, spread = slots(flip(z, g))
        picks = [jnp.transpose(spread(hit)).astype(BF16) for hit in hits]
        for c in range(0, width, tile):
            rows_in = ret[g, :, :, c : c + tile].reshape(per_plane * cap, tile)
            resid[:, c : c + tile] += sum(
                gate * dot(pick, rows_in) for gate, pick in zip(gate_cols, picks)
            )
        return carry

    lax.fori_loop(0, planes, combine, 0)
    out[...] = resid[...].astype(BF16)

    def drain(g, carry):
        wait_group(send, g, out_sem)
        wait_group(outb, g, back_sem)
        return carry

    lax.fori_loop(0, planes, drain, 0)


def fused(
    tp_size, planes, per_plane, cap,
    stream, outer_gate, inner_gate, conv_values, doc_ids, conv_taps, out_weight, norm_gain,
    route_ids, route_logits, group_weight, w_gate, w_up, w_down,
):
    rows, width = stream.shape
    length, chan = inner_gate.shape
    ff = w_gate.shape[2]
    top = route_ids.shape[1]
    vmem = pl.BlockSpec(memory_space=pltpu.VMEM)
    anywhere = pl.BlockSpec(memory_space=pl.ANY)
    blocks = pltpu.VMEM((planes, per_plane, cap, width), BF16)
    dma = pltpu.SemaphoreType.DMA
    return pl.pallas_call(
        functools.partial(fused_kernel, tp_size, planes, per_plane, cap),
        out_shape=jax.ShapeDtypeStruct((rows, width), BF16),
        in_specs=[vmem] * 10 + [anywhere] * 4,
        out_specs=vmem,
        scratch_shapes=[
            pltpu.VMEM(out_weight.shape, BF16),
            pltpu.VMEM((width, ff), BF16),
            pltpu.VMEM((width, ff), BF16),
            pltpu.VMEM((ff, width), BF16),
            pltpu.VMEM((2, 16, chan), BF16),
            pltpu.VMEM((2, 16, chan), BF16),
            pltpu.VMEM((2, 1, length), jnp.int32),
            pltpu.VMEM((tp_size, rows, chan), BF16),
            pltpu.VMEM((rows, chan), BF16),
            pltpu.VMEM((rows, width), F32),
            pltpu.VMEM((rows, width), BF16),
            pltpu.VMEM((per_plane * cap, ff), BF16),
            blocks, blocks, blocks, blocks,
            dma((4,)), dma((4,)), dma((4,)), dma, dma, dma,
            dma((planes,)), dma((planes,)), dma((planes,)), dma((planes,)),
        ],
        compiler_params=pltpu.CompilerParams(
            collective_id=0, has_side_effects=True, vmem_limit_bytes=56 * 1024 * 1024
        ),
    )(
        stream, outer_gate, inner_gate, conv_values, doc_ids[None, :], conv_taps,
        norm_gain[None, :], route_ids.T, route_logits.T, group_weight[None, :],
        out_weight, w_gate, w_up, w_down,
    )


def body(*args):
    stream, route_ids = args[0], args[8]
    tp_size = lax.axis_size("tp")
    total = lax.axis_size("sp") * tp_size
    cap = 2 * stream.shape[0] * route_ids.shape[1] // total
    planes = 4
    per_plane = total // planes
    if tp_size != 2 or total % planes or cap % 16 or per_plane * cap != stream.shape[0]:
        return on_device(*args)
    return fused(tp_size, planes, per_plane, cap, *args)


def solution(mesh):
    placed = (
        P(("sp", "tp"), None),
        P("sp", "tp"),
        P("sp", "tp"),
        P("sp", "tp"),
        P("sp"),
        P(None, "tp"),
        P(),
        P(),
        P(("sp", "tp"), None),
        P(("sp", "tp"), None),
        P(("sp", "tp")),
        P(("sp", "tp"), None, None),
        P(("sp", "tp"), None, None),
        P(("sp", "tp"), None, None),
    )
    return jax.shard_map(
        body, mesh=mesh, in_specs=placed, out_specs=P(("sp", "tp"), None), check_vma=False
    )
```

```python
import functools

import jax
import jax.numpy as jnp
from jax import lax
from jax.experimental import pallas as pl
from jax.experimental.pallas import tpu as pltpu
from jax.sharding import PartitionSpec as P


def padded_2(shard, sides, width):
    for axis, dim in sides:
        size, length = (lax.axis_size(axis), shard.shape[dim])
        up = [(i, (i + 1) % size) for i in range(size - 1)]
        down = [(j, i) for i, j in up]
        last = lax.slice_in_dim(shard, length - width, length, axis=dim)
        leading = lax.slice_in_dim(shard, 0, width, axis=dim)
        before = lax.ppermute(last, axis, up)
        after = lax.ppermute(leading, axis, down)
        shard = jnp.concatenate([before, shard, after], axis=dim)
    return shard


def on_device(
    stream,
    outer_gate,
    inner_gate,
    conv_values,
    doc_ids,
    conv_taps,
    out_weight,
    norm_gain,
    route_ids,
    route_logits,
    group_weight,
    w_gate,
    w_up,
    w_down,
):
    tok_rows = stream.shape[0]
    width = stream.shape[1]
    product = (inner_gate.astype(jnp.float32) * conv_values.astype(jnp.float32)).astype(
        jnp.bfloat16
    )
    doc_float = doc_ids.astype(jnp.bfloat16)
    padded, padded_docs = (padded_2(product, (("sp", 0),), 1), padded_2(doc_float, (("sp", 0),), 1))
    same_prev = (padded_docs[:-2] == doc_float).astype(jnp.float32)[:, None]
    same_next = (padded_docs[2:] == doc_float).astype(jnp.float32)[:, None]
    conv = (
        conv_taps[0] * padded[:-2].astype(jnp.float32) * same_prev
        + conv_taps[1] * product.astype(jnp.float32)
        + conv_taps[2] * padded[2:].astype(jnp.float32) * same_next
    )
    mixed = (outer_gate.astype(jnp.float32) * conv).astype(jnp.bfloat16)
    channels = lax.all_to_all(mixed, "tp", split_axis=0, concat_axis=1, tiled=True)
    projected = jnp.dot(channels, out_weight, preferred_element_type=jnp.float32)
    resid = stream.astype(jnp.float32) + projected
    scale = lax.rsqrt(jnp.mean(resid * resid, axis=-1, keepdims=True) + 1e-06)
    normed = (resid * scale * norm_gain).astype(jnp.bfloat16)
    expert_total = lax.axis_size("sp") * lax.axis_size("tp")
    top_count = route_ids.shape[1]
    capacity = 2 * tok_rows * top_count // expert_total
    flat_ids = route_ids.reshape(-1)
    one_hot = (flat_ids[:, None] == jnp.arange(expert_total, dtype=jnp.int32)[None, :]).astype(
        jnp.int32
    )
    rank = jnp.sum((jnp.cumsum(one_hot, axis=0) - 1) * one_hot, axis=1)
    slot = flat_ids * capacity + rank
    slot_count = expert_total * capacity
    source_row = (
        jnp.zeros((slot_count,), jnp.int32)
        .at[slot]
        .set(jnp.arange(flat_ids.shape[0], dtype=jnp.int32) // top_count)
    )
    filled = jnp.zeros((slot_count,), jnp.bool_).at[slot].set(True)
    outgoing = jnp.where(filled[:, None], normed[source_row], jnp.zeros((), jnp.bfloat16)).reshape(
        expert_total, capacity, width
    )
    arrived = lax.all_to_all(outgoing, ("sp", "tp"), split_axis=0, concat_axis=0, tiled=True)
    sources, items, features = arrived.shape
    rows_in = arrived.reshape(sources * items, features)
    hidden = (
        jax.nn.silu(jnp.dot(rows_in, w_gate[0], preferred_element_type=jnp.float32))
        * jnp.dot(rows_in, w_up[0], preferred_element_type=jnp.float32)
    ).astype(jnp.bfloat16)
    outputs = jnp.dot(hidden, w_down[0], preferred_element_type=jnp.float32).astype(jnp.bfloat16)
    returned = lax.all_to_all(
        outputs.reshape(sources, items, features),
        ("sp", "tp"),
        split_axis=0,
        concat_axis=0,
        tiled=True,
    )
    picked = (
        returned.reshape(slot_count, width)[slot]
        .astype(jnp.float32)
        .reshape(tok_rows, top_count, width)
    )
    expo = jnp.exp(route_logits)
    gate = group_weight[:, None] * expo / jnp.sum(expo, axis=1, keepdims=True)
    result = resid + jnp.sum(gate[:, :, None] * picked, axis=1)
    return result.astype(jnp.bfloat16)


MESH = pl.DeviceIdType.MESH
F32, BF16 = jnp.float32, jnp.bfloat16


def dot(a, b):
    return jnp.dot(a, b, preferred_element_type=F32)


PARTS = 4


def near(z, h):
    return 2 * (z // 2) + (z % 2 + h) % 2


def across(z):
    return 2 * ((z // 2 + 1) % 2) + z % 2


def fused_kernel(
    tp_size, planes, per_plane, cap,
    stream, outer, inner, values, docs, taps, gain, ids, logits, weight,
    ow_hbm, wg_hbm, wu_hbm, wd_hbm,
    out,
    ow, wg, wu, wd, edge_out, edge_in, doc_in, mix, mix_in, resid, normed, hidden,
    send, recv, outb, ret, far, far_ids, far_logits, far_weight, halves, part_in,
    load_sem, edge_send, edge_recv, mix_send, mix_recv, self_sem, self_back,
    out_sem, in_sem, back_sem, home_sem, far_send, far_recv, part_send, part_recv,
):
    sp, tp = lax.axis_index("sp"), lax.axis_index("tp")
    sp_size = planes * per_plane // tp_size
    total = planes * per_plane
    me = sp * tp_size + tp
    z, p = me // per_plane, me % per_plane
    rows, width = stream.shape
    chan = inner.shape[1]
    length = inner.shape[0]

    def place(index):
        return (index // tp_size, index % tp_size)

    loads = [
        pltpu.make_async_copy(src, dst, load_sem.at[i])
        for i, (src, dst) in enumerate(
            ((ow_hbm, ow), (wg_hbm.at[0], wg), (wu_hbm.at[0], wu), (wd_hbm.at[0], wd))
        )
    ]
    for load in loads:
        load.start()

    barrier = pltpu.get_barrier_semaphore()

    def greet(i, carry):
        pl.semaphore_signal(
            barrier, inc=1, device_id=place((me + i) % total), device_id_type=MESH
        )
        return carry

    lax.fori_loop(1, total, greet, 0)
    product = (inner[...].astype(F32) * values[...].astype(F32)).astype(BF16)
    edge_out[0] = product[:16]
    edge_out[1] = product[length - 16 :]
    pl.semaphore_wait(barrier, total - 1)

    left, right = ((sp + sp_size - 1) % sp_size, tp), ((sp + 1) % sp_size, tp)
    edges = []
    for side, (dest, src) in enumerate(((right, edge_out.at[1]), (left, edge_out.at[0]))):
        for kind, (source, target) in enumerate(
            ((src, edge_in.at[side]), (docs, doc_in.at[side]))
        ):
            edges.append(
                pltpu.make_async_remote_copy(
                    src_ref=source,
                    dst_ref=target,
                    send_sem=edge_send.at[2 * side + kind],
                    recv_sem=edge_recv.at[2 * side + kind],
                    device_id=dest,
                    device_id_type=MESH,
                )
            )
    for edge in edges:
        edge.start()

    mirror = place(across(z) * per_plane + p)

    def to_mirror(src, dst, source_sem, target_sem):
        return pltpu.make_async_remote_copy(
            src_ref=src,
            dst_ref=dst,
            send_sem=source_sem,
            recv_sem=target_sem,
            device_id=mirror,
            device_id_type=MESH,
        )

    routes = [
        to_mirror(src, dst, far_send.at[i], far_recv.at[i])
        for i, (src, dst) in enumerate(
            ((ids, far_ids), (logits, far_logits), (weight, far_weight))
        )
    ]
    for route in routes:
        route.start()

    top = ids.shape[0]

    def gate_columns(logit, group):
        expo = jnp.exp(logit[...])
        gates = group[...] * expo / jnp.sum(expo, axis=0, keepdims=True)
        return [
            jnp.transpose(jnp.broadcast_to(gates[k : k + 1], (rows, rows)))[:, :1]
            for k in range(top)
        ]

    before = (
        lax.broadcasted_iota(jnp.int32, (rows, rows), 0)
        < lax.broadcasted_iota(jnp.int32, (rows, rows), 1)
    ).astype(F32).astype(BF16)
    rank_of = lax.broadcasted_iota(jnp.int32, (per_plane, cap, rows), 1).astype(F32)

    def slots(plane, named_ids):
        id_rows = [named_ids[k : k + 1, :] for k in range(top)]
        expert = lax.broadcasted_iota(jnp.int32, (per_plane, rows), 0) + plane * per_plane
        hits = [(row == expert).astype(F32) for row in id_rows]
        named = sum(hits)
        ahead = dot(named.astype(BF16), before)

        def spread(hit):
            at = jnp.where(hit > 0, ahead, -1.0)
            grid = jnp.broadcast_to(at[:, None, :], (per_plane, cap, rows))
            return jnp.where(grid == rank_of, 1.0, 0.0).reshape(per_plane * cap, rows)

        return named, hits, spread

    for edge in edges:
        edge.wait()

    doc = jnp.broadcast_to(docs[...], (8, length))
    lane = lax.broadcasted_iota(jnp.int32, (8, length), 1)
    prior = jnp.where(
        lane == 0,
        pltpu.roll(jnp.broadcast_to(doc_in[0], (8, length)), 1, axis=1),
        pltpu.roll(doc, 1, axis=1),
    )
    later = jnp.where(
        lane == length - 1,
        pltpu.roll(jnp.broadcast_to(doc_in[1], (8, length)), length - 1, axis=1),
        pltpu.roll(doc, length - 1, axis=1),
    )
    spot = lane + sp * length
    same_prev = jnp.where((prior == doc) & (spot > 0), 1.0, 0.0)
    same_next = jnp.where((later == doc) & (spot < sp_size * length - 1), 1.0, 0.0)

    def column(row):
        return jnp.transpose(jnp.broadcast_to(row[:1], (128, length)))[:, :1]

    prod = product.astype(F32)
    row_at = lax.broadcasted_iota(jnp.int32, (length, chan), 0)
    prev = jnp.where(row_at == 0, edge_in[0].astype(F32)[15:16], pltpu.roll(prod, 1, axis=0))
    nxt = jnp.where(
        row_at == length - 1,
        edge_in[1].astype(F32)[:1],
        pltpu.roll(prod, length - 1, axis=0),
    )
    conv = (
        taps[0:1] * prev * column(same_prev)
        + taps[1:2] * prod
        + taps[2:3] * nxt * column(same_next)
    )
    mixed = (outer[...].astype(F32) * conv).astype(BF16)
    mix[...] = mixed.reshape(tp_size, rows, chan)
    other = 1 - tp
    swap = pltpu.make_async_remote_copy(
        src_ref=mix.at[other],
        dst_ref=mix_in,
        send_sem=mix_send,
        recv_sem=mix_recv,
        device_id=(sp, other),
        device_id_type=MESH,
    )
    swap.start()
    loads[0].wait()
    tile = 512
    own = mix[tp]
    for c in range(0, width, tile):
        resid[:, c : c + tile] = stream[:, c : c + tile].astype(F32) + dot(
            own, ow[pl.ds(pl.multiple_of(tp * chan, chan), chan), c : c + tile]
        )
    swap.wait()
    theirs = mix_in[...]
    squares = jnp.zeros((rows, 1), F32)
    for c in range(0, width, tile):
        part = resid[:, c : c + tile] + dot(
            theirs, ow[pl.ds(pl.multiple_of(other * chan, chan), chan), c : c + tile]
        )
        resid[:, c : c + tile] = part
        squares = squares + jnp.sum(part * part, axis=1, keepdims=True)
    scale = lax.rsqrt(squares / width + 1e-06)
    for c in range(0, width, tile):
        normed[:, c : c + tile] = (
            resid[:, c : c + tile] * scale * gain[:, c : c + tile]
        ).astype(BF16)

    def start_group(src, dst, h, source_sem, target_sem):
        def one(i, carry):
            peer = (p + i) % per_plane
            pltpu.make_async_remote_copy(
                src_ref=src.at[peer],
                dst_ref=dst.at[p],
                send_sem=source_sem,
                recv_sem=target_sem,
                device_id=place(near(z, h) * per_plane + peer),
                device_id_type=MESH,
            ).start()
            return carry

        lax.fori_loop(1 - h, per_plane, one, 0)

    def wait_group(buf, h, sem):
        span = buf if h else buf.at[pl.ds(0, per_plane - 1)]
        pltpu.make_async_copy(span, span, sem).wait()

    def keep_in(q):
        return pltpu.make_async_copy(send.at[2 * q, p], recv.at[2 * q, p], self_sem.at[q])

    def keep_back(q, c):
        return pltpu.make_async_copy(
            outb.at[c, 2 * q, p], ret.at[c, 2 * q, p], self_back.at[PARTS * q + c]
        )

    tile = width // PARTS

    def dispatch(q, h, source, named_ids):
        g = 2 * q + h
        named, hits, spread = slots(near(z, h), named_ids)
        pick = spread(named).astype(BF16)
        for c in range(0, width, tile):
            send[g, :, :, c : c + tile] = (
                dot(pick, source[:, c : c + tile])
                .astype(BF16)
                .reshape(per_plane, cap, tile)
            )
        start_group(send.at[g], recv.at[g], h, out_sem.at[g], in_sem.at[g])
        if h == 0:
            keep_in(q).start()

    def experts(q, each):
        keep_in(q).wait()
        for h in range(2):
            wait_group(recv.at[2 * q + h], h, in_sem.at[2 * q + h])
        count = 2 * per_plane * cap
        x = recv[2 * q : 2 * q + 2].reshape(count, width)
        ff = hidden.shape[1]
        for f in range(0, ff, 256):
            a = dot(x, wg[:, f : f + 256])
            b = dot(x, wu[:, f : f + 256])
            hidden[:, f : f + 256] = (a / (1.0 + jnp.exp(-a)) * b).astype(BF16)
        for c in range(PARTS):
            outb[c, 2 * q : 2 * q + 2] = (
                dot(hidden[...], wd[:, c * tile : (c + 1) * tile])
                .astype(BF16)
                .reshape(2, per_plane, cap, tile)
            )
            each(q, c)

    def give_back(q, c):
        for h in (1, 0):
            g, at = 2 * q + h, 4 * c + 2 * q + h
            start_group(outb.at[c, g], ret.at[c, g], h, back_sem.at[at], home_sem.at[at])
        keep_back(q, c).start()

    def take_back(q, c):
        keep_back(q, c).wait()
        for h in range(2):
            wait_group(ret.at[c, 2 * q + h], h, home_sem.at[4 * c + 2 * q + h])

    def picks_of(named_ids):
        spreads = [slots(near(z, h), named_ids) for h in range(2)]
        return [
            jnp.concatenate(
                [jnp.transpose(spread(hits[k])) for _, hits, spread in spreads], axis=1
            ).astype(BF16)
            for k in range(top)
        ]

    def combined(q, c, picks, gates):
        given = ret[c, 2 * q : 2 * q + 2].reshape(2 * per_plane * cap, tile)
        return sum(gate * dot(pick, given) for gate, pick in zip(gates, picks))

    dispatch(0, 1, normed, ids)
    whole = to_mirror(normed, far, far_send.at[3], far_recv.at[3])
    whole.start()
    dispatch(0, 0, normed, ids)
    for load in loads[1:]:
        load.wait()
    for route in routes:
        route.wait()

    experts(0, lambda q, c: None)
    whole.wait()
    dispatch(1, 1, far, far_ids)
    dispatch(1, 0, far, far_ids)
    for c in range(PARTS):
        give_back(0, c)
    far_picks, far_gates = picks_of(far_ids), gate_columns(far_logits, far_weight)
    experts(1, give_back)

    parts = [
        to_mirror(halves.at[c], part_in.at[c], part_send.at[c], part_recv.at[c])
        for c in range(PARTS)
    ]
    for c in range(PARTS):
        take_back(1, c)
        halves[c] = combined(1, c, far_picks, far_gates).astype(BF16)
        parts[c].start()
    picks, gates = picks_of(ids), gate_columns(logits, weight)
    for c in range(PARTS):
        take_back(0, c)
        resid[:, c * tile : (c + 1) * tile] += combined(0, c, picks, gates)
    for c in range(PARTS):
        parts[c].wait()
        out[:, c * tile : (c + 1) * tile] = (
            resid[:, c * tile : (c + 1) * tile] + part_in[c].astype(F32)
        ).astype(BF16)

    for g in range(4):
        wait_group(send.at[g], g % 2, out_sem.at[g])
        for c in range(PARTS):
            wait_group(outb.at[c, g], g % 2, back_sem.at[4 * c + g])


def fused(
    tp_size, planes, per_plane, cap,
    stream, outer_gate, inner_gate, conv_values, doc_ids, conv_taps, out_weight, norm_gain,
    route_ids, route_logits, group_weight, w_gate, w_up, w_down,
):
    rows, width = stream.shape
    length, chan = inner_gate.shape
    ff = w_gate.shape[2]
    top = route_ids.shape[1]
    vmem = pl.BlockSpec(memory_space=pltpu.VMEM)
    anywhere = pl.BlockSpec(memory_space=pl.ANY)
    blocks = pltpu.VMEM((4, per_plane, cap, width), BF16)
    cut = pltpu.VMEM((PARTS, 4, per_plane, cap, width // PARTS), BF16)
    slab = pltpu.VMEM((PARTS, rows, width // PARTS), BF16)
    dma = pltpu.SemaphoreType.DMA
    return pl.pallas_call(
        functools.partial(fused_kernel, tp_size, planes, per_plane, cap),
        out_shape=jax.ShapeDtypeStruct((rows, width), BF16),
        in_specs=[vmem] * 10 + [anywhere] * 4,
        out_specs=vmem,
        scratch_shapes=[
            pltpu.VMEM(out_weight.shape, BF16),
            pltpu.VMEM((width, ff), BF16),
            pltpu.VMEM((width, ff), BF16),
            pltpu.VMEM((ff, width), BF16),
            pltpu.VMEM((2, 16, chan), BF16),
            pltpu.VMEM((2, 16, chan), BF16),
            pltpu.VMEM((2, 1, length), jnp.int32),
            pltpu.VMEM((tp_size, rows, chan), BF16),
            pltpu.VMEM((rows, chan), BF16),
            pltpu.VMEM((rows, width), F32),
            pltpu.VMEM((rows, width), BF16),
            pltpu.VMEM((2 * per_plane * cap, ff), BF16),
            blocks, blocks, cut, cut,
            pltpu.VMEM((rows, width), BF16),
            pltpu.VMEM((top, rows), jnp.int32),
            pltpu.VMEM((top, rows), F32),
            pltpu.VMEM((1, rows), F32),
            slab, slab,
            dma((4,)), dma((4,)), dma((4,)), dma, dma, dma((2,)), dma((2 * PARTS,)),
            dma((4,)), dma((4,)), dma((4 * PARTS,)), dma((4 * PARTS,)),
            dma((4,)), dma((4,)), dma((PARTS,)), dma((PARTS,)),
        ],
        compiler_params=pltpu.CompilerParams(
            collective_id=0, has_side_effects=True, vmem_limit_bytes=56 * 1024 * 1024
        ),
    )(
        stream, outer_gate, inner_gate, conv_values, doc_ids[None, :], conv_taps,
        norm_gain[None, :], route_ids.T, route_logits.T, group_weight[None, :],
        out_weight, w_gate, w_up, w_down,
    )


def body(*args):
    stream, route_ids = args[0], args[8]
    tp_size = lax.axis_size("tp")
    total = lax.axis_size("sp") * tp_size
    cap = 2 * stream.shape[0] * route_ids.shape[1] // total
    planes = 4
    per_plane = total // planes
    if tp_size != 2 or total % planes or cap % 16 or per_plane * cap != stream.shape[0]:
        return on_device(*args)
    return fused(tp_size, planes, per_plane, cap, *args)


def solution(mesh):
    placed = (
        P(("sp", "tp"), None),
        P("sp", "tp"),
        P("sp", "tp"),
        P("sp", "tp"),
        P("sp"),
        P(None, "tp"),
        P(),
        P(),
        P(("sp", "tp"), None),
        P(("sp", "tp"), None),
        P(("sp", "tp")),
        P(("sp", "tp"), None, None),
        P(("sp", "tp"), None, None),
        P(("sp", "tp"), None, None),
    )
    return jax.shard_map(
        body, mesh=mesh, in_specs=placed, out_specs=P(("sp", "tp"), None), check_vma=False
    )
```

```python
import functools

import jax
import jax.numpy as jnp
from jax import lax
from jax.experimental import pallas as pl
from jax.experimental.pallas import tpu as pltpu
from jax.sharding import PartitionSpec as P


def padded_2(shard, sides, width):
    for axis, dim in sides:
        size, length = (lax.axis_size(axis), shard.shape[dim])
        up = [(i, (i + 1) % size) for i in range(size - 1)]
        down = [(j, i) for i, j in up]
        last = lax.slice_in_dim(shard, length - width, length, axis=dim)
        leading = lax.slice_in_dim(shard, 0, width, axis=dim)
        before = lax.ppermute(last, axis, up)
        after = lax.ppermute(leading, axis, down)
        shard = jnp.concatenate([before, shard, after], axis=dim)
    return shard


def on_device(
    stream,
    outer_gate,
    inner_gate,
    conv_values,
    doc_ids,
    conv_taps,
    out_weight,
    norm_gain,
    route_ids,
    route_logits,
    group_weight,
    w_gate,
    w_up,
    w_down,
):
    tok_rows = stream.shape[0]
    width = stream.shape[1]
    product = (inner_gate.astype(jnp.float32) * conv_values.astype(jnp.float32)).astype(
        jnp.bfloat16
    )
    doc_float = doc_ids.astype(jnp.bfloat16)
    padded, padded_docs = (padded_2(product, (("sp", 0),), 1), padded_2(doc_float, (("sp", 0),), 1))
    same_prev = (padded_docs[:-2] == doc_float).astype(jnp.float32)[:, None]
    same_next = (padded_docs[2:] == doc_float).astype(jnp.float32)[:, None]
    conv = (
        conv_taps[0] * padded[:-2].astype(jnp.float32) * same_prev
        + conv_taps[1] * product.astype(jnp.float32)
        + conv_taps[2] * padded[2:].astype(jnp.float32) * same_next
    )
    mixed = (outer_gate.astype(jnp.float32) * conv).astype(jnp.bfloat16)
    channels = lax.all_to_all(mixed, "tp", split_axis=0, concat_axis=1, tiled=True)
    projected = jnp.dot(channels, out_weight, preferred_element_type=jnp.float32)
    resid = stream.astype(jnp.float32) + projected
    scale = lax.rsqrt(jnp.mean(resid * resid, axis=-1, keepdims=True) + 1e-06)
    normed = (resid * scale * norm_gain).astype(jnp.bfloat16)
    expert_total = lax.axis_size("sp") * lax.axis_size("tp")
    top_count = route_ids.shape[1]
    capacity = 2 * tok_rows * top_count // expert_total
    flat_ids = route_ids.reshape(-1)
    one_hot = (flat_ids[:, None] == jnp.arange(expert_total, dtype=jnp.int32)[None, :]).astype(
        jnp.int32
    )
    rank = jnp.sum((jnp.cumsum(one_hot, axis=0) - 1) * one_hot, axis=1)
    slot = flat_ids * capacity + rank
    slot_count = expert_total * capacity
    source_row = (
        jnp.zeros((slot_count,), jnp.int32)
        .at[slot]
        .set(jnp.arange(flat_ids.shape[0], dtype=jnp.int32) // top_count)
    )
    filled = jnp.zeros((slot_count,), jnp.bool_).at[slot].set(True)
    outgoing = jnp.where(filled[:, None], normed[source_row], jnp.zeros((), jnp.bfloat16)).reshape(
        expert_total, capacity, width
    )
    arrived = lax.all_to_all(outgoing, ("sp", "tp"), split_axis=0, concat_axis=0, tiled=True)
    sources, items, features = arrived.shape
    rows_in = arrived.reshape(sources * items, features)
    hidden = (
        jax.nn.silu(jnp.dot(rows_in, w_gate[0], preferred_element_type=jnp.float32))
        * jnp.dot(rows_in, w_up[0], preferred_element_type=jnp.float32)
    ).astype(jnp.bfloat16)
    outputs = jnp.dot(hidden, w_down[0], preferred_element_type=jnp.float32).astype(jnp.bfloat16)
    returned = lax.all_to_all(
        outputs.reshape(sources, items, features),
        ("sp", "tp"),
        split_axis=0,
        concat_axis=0,
        tiled=True,
    )
    picked = (
        returned.reshape(slot_count, width)[slot]
        .astype(jnp.float32)
        .reshape(tok_rows, top_count, width)
    )
    expo = jnp.exp(route_logits)
    gate = group_weight[:, None] * expo / jnp.sum(expo, axis=1, keepdims=True)
    result = resid + jnp.sum(gate[:, :, None] * picked, axis=1)
    return result.astype(jnp.bfloat16)


MESH = pl.DeviceIdType.MESH
F32, BF16 = jnp.float32, jnp.bfloat16


def dot(a, b):
    return jnp.dot(a, b, preferred_element_type=F32)


PARTS = 4


def near(z, h):
    return 2 * (z // 2) + (z % 2 + h) % 2


def across(z):
    return 2 * ((z // 2 + 1) % 2) + z % 2


def fused_kernel(
    tp_size, planes, per_plane, cap,
    stream, outer, inner, values, docs, taps, gain, ids, logits, weight,
    ow_hbm, wg_hbm, wu_hbm, wd_hbm,
    out,
    ow, wg, wu, wd, edge_out, edge_in, doc_in, mix, mix_in, resid, normed, hidden,
    send, recv, outb, ret, far, far_ids, far_logits, far_weight, halves, part_in,
    load_sem, edge_send, edge_recv, mix_send, mix_recv, self_sem, self_back,
    out_sem, in_sem, back_sem, home_sem, far_send, far_recv, part_send, part_recv,
):
    sp, tp = lax.axis_index("sp"), lax.axis_index("tp")
    sp_size = planes * per_plane // tp_size
    total = planes * per_plane
    me = sp * tp_size + tp
    z, p = me // per_plane, me % per_plane
    rows, width = stream.shape
    chan = inner.shape[1]
    length = inner.shape[0]

    def place(index):
        return (index // tp_size, index % tp_size)

    loads = [
        pltpu.make_async_copy(src, dst, load_sem.at[i])
        for i, (src, dst) in enumerate(
            ((ow_hbm, ow), (wg_hbm.at[0], wg), (wu_hbm.at[0], wu), (wd_hbm.at[0], wd))
        )
    ]
    for load in loads:
        load.start()

    barrier = pltpu.get_barrier_semaphore()

    def greet(i, carry):
        pl.semaphore_signal(
            barrier, inc=1, device_id=place((me + i) % total), device_id_type=MESH
        )
        return carry

    lax.fori_loop(1, total, greet, 0)
    product = (inner[...].astype(F32) * values[...].astype(F32)).astype(BF16)
    edge_out[0] = product[:16]
    edge_out[1] = product[length - 16 :]
    pl.semaphore_wait(barrier, total - 1)

    left, right = ((sp + sp_size - 1) % sp_size, tp), ((sp + 1) % sp_size, tp)
    edges = []
    for side, (dest, src) in enumerate(((right, edge_out.at[1]), (left, edge_out.at[0]))):
        for kind, (source, target) in enumerate(
            ((src, edge_in.at[side]), (docs, doc_in.at[side]))
        ):
            edges.append(
                pltpu.make_async_remote_copy(
                    src_ref=source,
                    dst_ref=target,
                    send_sem=edge_send.at[2 * side + kind],
                    recv_sem=edge_recv.at[2 * side + kind],
                    device_id=dest,
                    device_id_type=MESH,
                )
            )
    for edge in edges:
        edge.start()

    mirror = place(across(z) * per_plane + p)

    def to_mirror(src, dst, source_sem, target_sem):
        return pltpu.make_async_remote_copy(
            src_ref=src,
            dst_ref=dst,
            send_sem=source_sem,
            recv_sem=target_sem,
            device_id=mirror,
            device_id_type=MESH,
        )

    routes = [
        to_mirror(src, dst, far_send.at[i], far_recv.at[i])
        for i, (src, dst) in enumerate(
            ((ids, far_ids), (logits, far_logits), (weight, far_weight))
        )
    ]
    for route in routes:
        route.start()

    top = ids.shape[0]

    def gate_columns(logit, group):
        expo = jnp.exp(logit[...])
        gates = group[...] * expo / jnp.sum(expo, axis=0, keepdims=True)
        return [
            jnp.transpose(jnp.broadcast_to(gates[k : k + 1], (rows, rows)))[:, :1]
            for k in range(top)
        ]

    before = (
        lax.broadcasted_iota(jnp.int32, (rows, rows), 0)
        < lax.broadcasted_iota(jnp.int32, (rows, rows), 1)
    ).astype(F32).astype(BF16)
    rank_of = lax.broadcasted_iota(jnp.int32, (per_plane, cap, rows), 1).astype(F32)

    def slots(plane, named_ids):
        id_rows = [named_ids[k : k + 1, :] for k in range(top)]
        expert = lax.broadcasted_iota(jnp.int32, (per_plane, rows), 0) + plane * per_plane
        hits = [(row == expert).astype(F32) for row in id_rows]
        named = sum(hits)
        ahead = dot(named.astype(BF16), before)

        def spread(hit):
            at = jnp.where(hit > 0, ahead, -1.0)
            grid = jnp.broadcast_to(at[:, None, :], (per_plane, cap, rows))
            return jnp.where(grid == rank_of, 1.0, 0.0).reshape(per_plane * cap, rows)

        return named, hits, spread

    for edge in edges:
        edge.wait()

    doc = jnp.broadcast_to(docs[...], (8, length))
    lane = lax.broadcasted_iota(jnp.int32, (8, length), 1)
    prior = jnp.where(
        lane == 0,
        pltpu.roll(jnp.broadcast_to(doc_in[0], (8, length)), 1, axis=1),
        pltpu.roll(doc, 1, axis=1),
    )
    later = jnp.where(
        lane == length - 1,
        pltpu.roll(jnp.broadcast_to(doc_in[1], (8, length)), length - 1, axis=1),
        pltpu.roll(doc, length - 1, axis=1),
    )
    spot = lane + sp * length
    same_prev = jnp.where((prior == doc) & (spot > 0), 1.0, 0.0)
    same_next = jnp.where((later == doc) & (spot < sp_size * length - 1), 1.0, 0.0)

    def column(row):
        return jnp.transpose(jnp.broadcast_to(row[:1], (128, length)))[:, :1]

    prod = product.astype(F32)
    row_at = lax.broadcasted_iota(jnp.int32, (length, chan), 0)
    prev = jnp.where(row_at == 0, edge_in[0].astype(F32)[15:16], pltpu.roll(prod, 1, axis=0))
    nxt = jnp.where(
        row_at == length - 1,
        edge_in[1].astype(F32)[:1],
        pltpu.roll(prod, length - 1, axis=0),
    )
    conv = (
        taps[0:1] * prev * column(same_prev)
        + taps[1:2] * prod
        + taps[2:3] * nxt * column(same_next)
    )
    mixed = (outer[...].astype(F32) * conv).astype(BF16)
    mix[...] = mixed.reshape(tp_size, rows, chan)
    other = 1 - tp
    swap = pltpu.make_async_remote_copy(
        src_ref=mix.at[other],
        dst_ref=mix_in,
        send_sem=mix_send,
        recv_sem=mix_recv,
        device_id=(sp, other),
        device_id_type=MESH,
    )
    swap.start()
    loads[0].wait()
    tile = 512
    own = mix[tp]
    for c in range(0, width, tile):
        resid[:, c : c + tile] = stream[:, c : c + tile].astype(F32) + dot(
            own, ow[pl.ds(pl.multiple_of(tp * chan, chan), chan), c : c + tile]
        )
    swap.wait()
    theirs = mix_in[...]
    squares = jnp.zeros((rows, 1), F32)
    for c in range(0, width, tile):
        part = resid[:, c : c + tile] + dot(
            theirs, ow[pl.ds(pl.multiple_of(other * chan, chan), chan), c : c + tile]
        )
        resid[:, c : c + tile] = part
        squares = squares + jnp.sum(part * part, axis=1, keepdims=True)
    scale = lax.rsqrt(squares / width + 1e-06)
    for c in range(0, width, tile):
        normed[:, c : c + tile] = (
            resid[:, c : c + tile] * scale * gain[:, c : c + tile]
        ).astype(BF16)

    def start_group(src, dst, h, source_sem, target_sem):
        def one(i, carry):
            peer = (p + i) % per_plane
            pltpu.make_async_remote_copy(
                src_ref=src.at[peer],
                dst_ref=dst.at[p],
                send_sem=source_sem,
                recv_sem=target_sem,
                device_id=place(near(z, h) * per_plane + peer),
                device_id_type=MESH,
            ).start()
            return carry

        lax.fori_loop(1 - h, per_plane, one, 0)

    def wait_group(buf, h, sem):
        span = buf if h else buf.at[pl.ds(0, per_plane - 1)]
        pltpu.make_async_copy(span, span, sem).wait()

    def keep_in(q):
        return pltpu.make_async_copy(send.at[2 * q, p], recv.at[2 * q, p], self_sem.at[q])

    def keep_back(q, c):
        return pltpu.make_async_copy(
            outb.at[c, 2 * q, p], ret.at[c, 2 * q, p], self_back.at[PARTS * q + c]
        )

    tile = width // PARTS

    def dispatch(q, h, source, named_ids):
        g = 2 * q + h
        named, hits, spread = slots(near(z, h), named_ids)
        pick = spread(named).astype(BF16)
        for c in range(0, width, tile):
            send[g, :, :, c : c + tile] = (
                dot(pick, source[:, c : c + tile])
                .astype(BF16)
                .reshape(per_plane, cap, tile)
            )
        start_group(send.at[g], recv.at[g], h, out_sem.at[g], in_sem.at[g])
        if h == 0:
            keep_in(q).start()

    def experts(q, each):
        keep_in(q).wait()
        for h in range(2):
            wait_group(recv.at[2 * q + h], h, in_sem.at[2 * q + h])
        count = 2 * per_plane * cap
        x = recv[2 * q : 2 * q + 2].reshape(count, width)
        ff = hidden.shape[1]
        for f in range(0, ff, 256):
            a = dot(x, wg[:, f : f + 256])
            b = dot(x, wu[:, f : f + 256])
            hidden[:, f : f + 256] = (a / (1.0 + jnp.exp(-a)) * b).astype(BF16)
        for c in range(PARTS):
            outb[c, 2 * q : 2 * q + 2] = (
                dot(hidden[...], wd[:, c * tile : (c + 1) * tile])
                .astype(BF16)
                .reshape(2, per_plane, cap, tile)
            )
            each(q, c)

    def give_back(q, c):
        for h in (1, 0):
            g, at = 2 * q + h, 4 * c + 2 * q + h
            start_group(outb.at[c, g], ret.at[c, g], h, back_sem.at[at], home_sem.at[at])
        keep_back(q, c).start()

    def take_back(q, c):
        keep_back(q, c).wait()
        for h in range(2):
            wait_group(ret.at[c, 2 * q + h], h, home_sem.at[4 * c + 2 * q + h])

    def picks_of(named_ids):
        spreads = [slots(near(z, h), named_ids) for h in range(2)]
        return [
            jnp.concatenate(
                [jnp.transpose(spread(hits[k])) for _, hits, spread in spreads], axis=1
            ).astype(BF16)
            for k in range(top)
        ]

    def combined(q, c, picks, gates):
        given = ret[c, 2 * q : 2 * q + 2].reshape(2 * per_plane * cap, tile)
        return sum(gate * dot(pick, given) for gate, pick in zip(gates, picks))

    dispatch(0, 1, normed, ids)
    whole = to_mirror(normed, far, far_send.at[3], far_recv.at[3])
    whole.start()
    dispatch(0, 0, normed, ids)
    for load in loads[1:]:
        load.wait()
    for route in routes:
        route.wait()

    experts(0, lambda q, c: None)
    whole.wait()
    dispatch(1, 1, far, far_ids)
    dispatch(1, 0, far, far_ids)
    far_picks, far_gates = picks_of(far_ids), gate_columns(far_logits, far_weight)
    experts(1, give_back)
    for c in range(PARTS):
        give_back(0, c)

    parts = [
        to_mirror(halves.at[c], part_in.at[c], part_send.at[c], part_recv.at[c])
        for c in range(PARTS)
    ]
    for c in range(PARTS):
        take_back(1, c)
        halves[c] = combined(1, c, far_picks, far_gates).astype(BF16)
        parts[c].start()
    picks, gates = picks_of(ids), gate_columns(logits, weight)
    for c in range(PARTS):
        take_back(0, c)
        resid[:, c * tile : (c + 1) * tile] += combined(0, c, picks, gates)
    for c in range(PARTS):
        parts[c].wait()
        out[:, c * tile : (c + 1) * tile] = (
            resid[:, c * tile : (c + 1) * tile] + part_in[c].astype(F32)
        ).astype(BF16)

    for g in range(4):
        wait_group(send.at[g], g % 2, out_sem.at[g])
        for c in range(PARTS):
            wait_group(outb.at[c, g], g % 2, back_sem.at[4 * c + g])


def fused(
    tp_size, planes, per_plane, cap,
    stream, outer_gate, inner_gate, conv_values, doc_ids, conv_taps, out_weight, norm_gain,
    route_ids, route_logits, group_weight, w_gate, w_up, w_down,
):
    rows, width = stream.shape
    length, chan = inner_gate.shape
    ff = w_gate.shape[2]
    top = route_ids.shape[1]
    vmem = pl.BlockSpec(memory_space=pltpu.VMEM)
    anywhere = pl.BlockSpec(memory_space=pl.ANY)
    blocks = pltpu.VMEM((4, per_plane, cap, width), BF16)
    cut = pltpu.VMEM((PARTS, 4, per_plane, cap, width // PARTS), BF16)
    slab = pltpu.VMEM((PARTS, rows, width // PARTS), BF16)
    dma = pltpu.SemaphoreType.DMA
    return pl.pallas_call(
        functools.partial(fused_kernel, tp_size, planes, per_plane, cap),
        out_shape=jax.ShapeDtypeStruct((rows, width), BF16),
        in_specs=[vmem] * 10 + [anywhere] * 4,
        out_specs=vmem,
        scratch_shapes=[
            pltpu.VMEM(out_weight.shape, BF16),
            pltpu.VMEM((width, ff), BF16),
            pltpu.VMEM((width, ff), BF16),
            pltpu.VMEM((ff, width), BF16),
            pltpu.VMEM((2, 16, chan), BF16),
            pltpu.VMEM((2, 16, chan), BF16),
            pltpu.VMEM((2, 1, length), jnp.int32),
            pltpu.VMEM((tp_size, rows, chan), BF16),
            pltpu.VMEM((rows, chan), BF16),
            pltpu.VMEM((rows, width), F32),
            pltpu.VMEM((rows, width), BF16),
            pltpu.VMEM((2 * per_plane * cap, ff), BF16),
            blocks, blocks, cut, cut,
            pltpu.VMEM((rows, width), BF16),
            pltpu.VMEM((top, rows), jnp.int32),
            pltpu.VMEM((top, rows), F32),
            pltpu.VMEM((1, rows), F32),
            slab, slab,
            dma((4,)), dma((4,)), dma((4,)), dma, dma, dma((2,)), dma((2 * PARTS,)),
            dma((4,)), dma((4,)), dma((4 * PARTS,)), dma((4 * PARTS,)),
            dma((4,)), dma((4,)), dma((PARTS,)), dma((PARTS,)),
        ],
        compiler_params=pltpu.CompilerParams(
            collective_id=0, has_side_effects=True, vmem_limit_bytes=56 * 1024 * 1024
        ),
    )(
        stream, outer_gate, inner_gate, conv_values, doc_ids[None, :], conv_taps,
        norm_gain[None, :], route_ids.T, route_logits.T, group_weight[None, :],
        out_weight, w_gate, w_up, w_down,
    )


def body(*args):
    stream, route_ids = args[0], args[8]
    tp_size = lax.axis_size("tp")
    total = lax.axis_size("sp") * tp_size
    cap = 2 * stream.shape[0] * route_ids.shape[1] // total
    planes = 4
    per_plane = total // planes
    if tp_size != 2 or total % planes or cap % 16 or per_plane * cap != stream.shape[0]:
        return on_device(*args)
    return fused(tp_size, planes, per_plane, cap, *args)


def solution(mesh):
    placed = (
        P(("sp", "tp"), None),
        P("sp", "tp"),
        P("sp", "tp"),
        P("sp", "tp"),
        P("sp"),
        P(None, "tp"),
        P(),
        P(),
        P(("sp", "tp"), None),
        P(("sp", "tp"), None),
        P(("sp", "tp")),
        P(("sp", "tp"), None, None),
        P(("sp", "tp"), None, None),
        P(("sp", "tp"), None, None),
    )
    return jax.shard_map(
        body, mesh=mesh, in_specs=placed, out_specs=P(("sp", "tp"), None), check_vma=False
    )
```
